32 devices in a mesh: sp: 4 (over z), tp: 8 (over y, x, core).
Axes of the slice: x: 2, y: 2, z: 4, core: 2. Of those that a mesh axis runs over, the one named last changes fastest.
Arguments:
- target_rows: bfloat16 [768, 2048], P(('sp', 'tp')), may hold values from -6 to 6
- source_rows: bfloat16 [4096, 2048], P(('sp', 'tp')), may hold values from -6 to 6
- target_gain: float32 [2048], replicated, may hold values from 0.55 to 9
- source_gain: float32 [2048], replicated, may hold values from 0.55 to 9
- query_weight: bfloat16 [2048, 2048], P(None, 'tp'), may hold values from -0.125 to 0.125
- key_weight: bfloat16 [2048, 512], P('tp'), may hold values from -0.125 to 0.125
- value_weight: bfloat16 [2048, 512], P('tp'), may hold values from -0.125 to 0.125
- out_weight: bfloat16 [2048, 2048], P('tp'), may hold values from -0.125 to 0.125
- out_cotangent: bfloat16 [768, 2048], P(('sp', 'tp')), may hold values from -6 to 6
Outputs:
- target_grad: float32 [768, 2048], P(('sp', 'tp'))
- source_grad: float32 [4096, 2048], P(('sp', 'tp'))
- out_weight_grad: float32 [2048, 2048], P('tp')
The draws below stay inside these ranges and needn't reach their ends.
All inputs are finite; a program needn't handle non-finite values.
Results may differ from the reference program's by a relative error of at most 0.03.
Values may be sent and summed in bfloat16 or wider, within the bound.
A program may use at most 64 MiB of HBM per device.

```python
import jax
import jax.numpy as jnp
from jax import lax

D = 2048
HEADS = 32
HEAD_DIM = 64
KV_HEADS = 8
TGT_ALL = 768
SRC_ALL = 4096


def gain_draw(seed_key):
    return 1.0 + 0.18 * jax.random.truncated_normal(seed_key, -2.5, 2.5, (D,), jnp.float32)


def draw_target_gain(key, part):
    return gain_draw(jax.random.fold_in(key, 11))


def draw_source_gain(key, part):
    return gain_draw(jax.random.fold_in(key, 23))


def steps_of(key, extent, cuts, least, largest):
    level = 1.0
    for axis_at, blocks in cuts:
        heights = jax.random.uniform(jax.random.fold_in(jax.random.fold_in(key, 6), axis_at), (blocks,), jnp.float32, least / len(cuts), largest / len(cuts))
        level = level * jnp.repeat(jnp.exp(heights), extent[axis_at] // blocks).reshape((-1,) + (1,) * (len(extent) - 1 - axis_at))
    return level


def scatter_about(key, extent, spread, bound, shards=(), kind=jnp.bfloat16):
    drawn = jax.random.normal(key, extent, jnp.float32) * spread
    if len(shards) > 0:
        drawn = steps_of(key, extent, shards, -0.22, 0.18) * drawn
    return jnp.clip(drawn, min=-bound, max=bound).astype(kind)


def setup_inputs(seed: int = 0) -> dict:
    streams_of = jax.random.split(jax.random.key(seed), 10)
    return {
        "target_rows": scatter_about(streams_of[0], (TGT_ALL, D), 1.0, 6.0, ((0, 32),)),
        "source_rows": scatter_about(streams_of[1], (SRC_ALL, D), 1.0, 6.0, ((0, 32),)),
        "target_gain": draw_target_gain(jax.random.fold_in(streams_of[9], 71), 0),
        "source_gain": draw_source_gain(jax.random.fold_in(streams_of[9], 71), 0),
        "query_weight": scatter_about(streams_of[4], (D, HEADS * HEAD_DIM), D ** -0.5, 0.125, ((1, 8),)),
        "key_weight": scatter_about(streams_of[5], (D, KV_HEADS * HEAD_DIM), D ** -0.5, 0.125, ((0, 8),)),
        "value_weight": scatter_about(streams_of[6], (D, KV_HEADS * HEAD_DIM), D ** -0.5, 0.125, ((0, 8),)),
        "out_weight": scatter_about(streams_of[7], (HEADS * HEAD_DIM, D), (HEADS * HEAD_DIM) ** -0.5, 0.125, ((0, 8),)),
        "out_cotangent": scatter_about(streams_of[8], (TGT_ALL, D), 1.0, 6.0, ((0, 32),)),
    }


EPSILON = 1e-06

def normalize(matrix, gain_vector):
    widened = matrix.astype(jnp.float32)
    factor = lax.rsqrt(lax.optimization_barrier(jnp.mean(widened * widened, axis=-1, keepdims=True)) + EPSILON)
    return (widened * factor * gain_vector).astype(jnp.bfloat16)

def norm_back(matrix, gain_vector, upstream):
    widened = matrix.astype(jnp.float32)
    factor = lax.rsqrt(lax.optimization_barrier(jnp.mean(widened * widened, axis=-1, keepdims=True)) + EPSILON)
    weighted = upstream * gain_vector
    inner_sum = lax.optimization_barrier(jnp.mean(weighted * widened, axis=-1, keepdims=True))
    return factor * weighted - widened * factor ** 3 * inner_sum

def reference(target_rows, source_rows, target_gain, source_gain, query_weight, key_weight, value_weight, out_weight, out_cotangent):
    score_scale = HEAD_DIM ** (-0.5)
    group_size = HEADS // KV_HEADS
    normed_t = normalize(target_rows, target_gain)
    normed_s = normalize(source_rows, source_gain)
    queries = jnp.dot(normed_t, query_weight, preferred_element_type=jnp.float32).astype(jnp.bfloat16)
    keys_all = jnp.dot(normed_s, key_weight, preferred_element_type=jnp.float32).astype(jnp.bfloat16)
    values_all = jnp.dot(normed_s, value_weight, preferred_element_type=jnp.float32).astype(jnp.bfloat16)
    query_heads = queries.reshape(TGT_ALL, HEADS, HEAD_DIM).transpose(1, 0, 2)
    key_heads = keys_all.reshape(SRC_ALL, KV_HEADS, HEAD_DIM).transpose(1, 0, 2)
    value_heads = values_all.reshape(SRC_ALL, KV_HEADS, HEAD_DIM).transpose(1, 0, 2)
    out_heads = out_weight.reshape(HEADS, HEAD_DIM, D)

    def one_head(head_index):
        query = query_heads[head_index]
        key_head = key_heads[head_index // group_size]
        value_head = value_heads[head_index // group_size]
        scores = jnp.dot(query, key_head.T, preferred_element_type=jnp.float32) * score_scale
        row_max = lax.optimization_barrier(jnp.max(scores, axis=1, keepdims=True))
        weights = jnp.exp(scores - row_max)
        total = lax.optimization_barrier(jnp.sum(weights, axis=1, keepdims=True))
        attended = (jnp.dot(weights.astype(jnp.bfloat16), value_head, preferred_element_type=jnp.float32) / total).astype(jnp.bfloat16)
        log_total = row_max + jnp.log(total)
        d_attended = jnp.dot(out_cotangent, out_heads[head_index].T, preferred_element_type=jnp.float32).astype(jnp.bfloat16)
        delta = lax.optimization_barrier(jnp.sum(d_attended.astype(jnp.float32) * attended.astype(jnp.float32), axis=1, keepdims=True))
        probs = jnp.exp(scores - log_total)
        d_value = jnp.dot(probs.astype(jnp.bfloat16).T, d_attended, preferred_element_type=jnp.float32)
        d_probs = jnp.dot(d_attended, value_head.T, preferred_element_type=jnp.float32)
        d_scores = (probs * (d_probs - delta)).astype(jnp.bfloat16)
        d_query = jnp.dot(d_scores, key_head, preferred_element_type=jnp.float32) * score_scale
        d_key = jnp.dot(d_scores.T, query, preferred_element_type=jnp.float32) * score_scale
        return (attended, d_query, d_key, d_value)
    attended, d_query, d_key, d_value = lax.map(one_head, jnp.arange(HEADS))
    key_sum = lax.optimization_barrier(jnp.sum(d_key.reshape(KV_HEADS, group_size, SRC_ALL, HEAD_DIM), axis=1))
    value_sum = lax.optimization_barrier(jnp.sum(d_value.reshape(KV_HEADS, group_size, SRC_ALL, HEAD_DIM), axis=1))
    key_grad = key_sum.transpose(1, 0, 2).reshape(SRC_ALL, KV_HEADS * HEAD_DIM).astype(jnp.bfloat16)
    value_grad = value_sum.transpose(1, 0, 2).reshape(SRC_ALL, KV_HEADS * HEAD_DIM).astype(jnp.bfloat16)
    attended_rows = attended.transpose(1, 0, 2).reshape(TGT_ALL, HEADS * HEAD_DIM)
    query_grad = d_query.transpose(1, 0, 2).reshape(TGT_ALL, HEADS * HEAD_DIM).astype(jnp.bfloat16)
    out_weight_grad = jnp.dot(attended_rows.T, out_cotangent, preferred_element_type=jnp.float32)
    d_normed_t = jnp.dot(query_grad, query_weight.T, preferred_element_type=jnp.float32)
    target_grad = out_cotangent.astype(jnp.float32) + norm_back(target_rows, target_gain, d_normed_t)
    d_normed_s = jnp.dot(key_grad, key_weight.T, preferred_element_type=jnp.float32) + jnp.dot(value_grad, value_weight.T, preferred_element_type=jnp.float32)
    source_grad = norm_back(source_rows, source_gain, d_normed_s)
    return (target_grad, source_grad, out_weight_grad)
```

```python
import functools

import jax
import jax.numpy as jnp
from jax import lax
from jax.experimental import pallas as pl
from jax.experimental.pallas import tpu as pltpu
from jax.sharding import PartitionSpec as P

HEAD_DIM = 64
KV_HEADS = 8
EPSILON = 1e-06
MESH = pl.DeviceIdType.MESH


def normalize(matrix, gain_vector):
    widened = matrix.astype(jnp.float32)
    factor = lax.rsqrt(jnp.mean(widened * widened, axis=-1, keepdims=True) + EPSILON)
    return (widened * factor * gain_vector).astype(jnp.bfloat16)


def norm_back(matrix, gain_vector, upstream):
    widened = matrix.astype(jnp.float32)
    factor = lax.rsqrt(jnp.mean(widened * widened, axis=-1, keepdims=True) + EPSILON)
    weighted = upstream * gain_vector
    inner_sum = jnp.mean(weighted * widened, axis=-1, keepdims=True)
    return factor * weighted - widened * factor**3 * inner_sum


def exchange_kernel(kinds, sp_n, tp_n, *refs):
    count = len(kinds)
    ins, outs = refs[:count], refs[count : 2 * count]
    send_sems, recv_sems = refs[2 * count : 3 * count], refs[3 * count :]
    sp_me, tp_me = lax.axis_index("sp"), lax.axis_index("tp")
    sizes, places = {"sp": sp_n, "tp": tp_n}, {"sp": sp_me, "tp": tp_me}

    def address(axis, peer):
        return (peer, tp_me) if axis == "sp" else (sp_me, peer)

    axes = sorted({kind.split("_")[1] for kind in kinds})
    barrier = pltpu.get_barrier_semaphore()
    for axis in axes:
        for k in range(1, sizes[axis]):
            peer = lax.rem(places[axis] + k, sizes[axis])
            pl.semaphore_signal(barrier, inc=1, device_id=address(axis, peer), device_id_type=MESH)
    pl.semaphore_wait(barrier, sum(sizes[axis] - 1 for axis in axes))

    def copy(i, axis, source, slot, k, peer):
        return pltpu.make_async_remote_copy(
            src_ref=source,
            dst_ref=outs[i].at[slot],
            send_sem=send_sems[i].at[k],
            recv_sem=recv_sems[i].at[slot],
            device_id=address(axis, peer),
            device_id_type=MESH,
        )

    sent = []
    for i, kind in enumerate(kinds):
        mode, axis = kind.split("_")
        n, me = sizes[axis], places[axis]
        if mode == "pair":
            partner = me + 1 - 2 * lax.rem(me, 2)
            for k in range(1, n // 2):
                sent.append(copy(i, axis, ins[i], me, k, lax.rem(me + 2 * k, n)))
                sent[-1].start()
            sent.append(copy(i, axis, ins[i], me, 0, partner))
            sent[-1].start()
        else:
            for k in range(1, n):
                peer = lax.rem(me + k, n)
                source = ins[i] if mode == "gather" else ins[i].at[peer]
                sent.append(copy(i, axis, source, me, k, peer))
                sent[-1].start()
    for i, kind in enumerate(kinds):
        mode, axis = kind.split("_")
        me = places[axis]
        outs[i][me] = ins[i][me] if mode == "swap" else ins[i][...]
    for i, kind in enumerate(kinds):
        mode, axis = kind.split("_")
        n, me = sizes[axis], places[axis]
        if mode == "pair":
            partner = me + 1 - 2 * lax.rem(me, 2)
            for k in range(1, n // 2):
                origin = lax.rem(me + n - 2 * k, n)
                passed = copy(i, axis, outs[i].at[origin], origin, n // 2 + k - 1, partner)
                passed.wait_recv()
                passed.start()
                sent.append(passed)
    for i, kind in enumerate(kinds):
        mode, axis = kind.split("_")
        n, me = sizes[axis], places[axis]
        if mode == "pair":
            partner = me + 1 - 2 * lax.rem(me, 2)
            for k in range(n // 2):
                origin = lax.rem(partner + n - 2 * k, n)
                copy(i, axis, outs[i].at[origin], origin, 0, partner).wait_recv()
        else:
            for k in range(1, n):
                origin = lax.rem(me + n - k, n)
                copy(i, axis, outs[i].at[origin], origin, 0, origin).wait_recv()
    for one in sent:
        one.wait_send()


def exchange(collective_id, *parts):
    sp_n, tp_n = lax.axis_size("sp"), lax.axis_size("tp")
    kinds = tuple(kind for kind, array in parts)
    arrays = [array for kind, array in parts]
    shapes, sends, recvs = [], [], []
    for kind, array in parts:
        mode, axis = kind.split("_")
        n = sp_n if axis == "sp" else tp_n
        shape = array.shape if mode == "swap" else (n,) + array.shape
        shapes.append(jax.ShapeDtypeStruct(shape, array.dtype))
        sends.append(pltpu.SemaphoreType.DMA((n,)))
        recvs.append(pltpu.SemaphoreType.DMA((n,)))
    return pl.pallas_call(
        functools.partial(exchange_kernel, kinds, sp_n, tp_n),
        out_shape=shapes,
        in_specs=[pl.BlockSpec(memory_space=pltpu.VMEM)] * len(parts),
        out_specs=[pl.BlockSpec(memory_space=pltpu.VMEM)] * len(parts),
        scratch_shapes=sends + recvs,
        compiler_params=pltpu.CompilerParams(
            collective_id=collective_id,
            has_side_effects=True,
            vmem_limit_bytes=56 * 1024 * 1024,
        ),
    )(*arrays)


def matmul(left, right):
    return jnp.dot(left, right, preferred_element_type=jnp.float32)


def einsum(text, left, right):
    return jnp.einsum(text, left, right, preferred_element_type=jnp.float32)


def body(
    target_rows,
    source_rows,
    target_gain,
    source_gain,
    query_weight,
    key_weight,
    value_weight,
    out_weight,
    out_cotangent,
):
    sp_n, tp_n = lax.axis_size("sp"), lax.axis_size("tp")
    width = target_rows.shape[1]
    local_width = query_weight.shape[1]
    local_heads = local_width // HEAD_DIM
    slot_heads = max(1, KV_HEADS // tp_n)
    copies = max(1, tp_n // KV_HEADS)
    per_slot = local_heads // slot_heads
    slot_width = slot_heads * HEAD_DIM
    score_scale = HEAD_DIM ** (-0.5)
    bf16 = jnp.bfloat16

    normed_t = normalize(target_rows, target_gain)
    normed_s = normalize(source_rows, source_gain)
    source_local = normed_s.shape[0]
    target_local = normed_t.shape[0]
    target_block = tp_n * target_local
    source_block = tp_n * source_local

    rows_in, cot_in, key_full, value_full, cot_column = exchange(
        0,
        ("pair_tp", normed_t),
        ("pair_tp", out_cotangent),
        ("pair_tp", key_weight),
        ("pair_tp", value_weight),
        ("gather_sp", out_cotangent),
    )
    key_full = key_full.reshape(width, -1)
    value_full = value_full.reshape(width, -1)
    queries = matmul(rows_in.reshape(target_block, width), query_weight).astype(bf16)
    d_attended = matmul(cot_in.reshape(target_block, width), out_weight.T).astype(bf16)
    key_own = matmul(normed_s, key_full).astype(bf16)
    value_own = matmul(normed_s, value_full).astype(bf16)

    def to_slots(matrix):
        split = matrix.reshape(source_local, tp_n // copies, 1, slot_width)
        spread = jnp.broadcast_to(split, (source_local, tp_n // copies, copies, slot_width))
        return spread.reshape(source_local, tp_n, slot_width).transpose(1, 0, 2)

    slots = jnp.concatenate([to_slots(key_own), to_slots(value_own)], axis=2)
    all_queries, all_grads, kv_block, cot_all = exchange(
        1,
        ("gather_sp", queries),
        ("gather_sp", d_attended),
        ("swap_tp", slots),
        ("pair_tp", cot_column),
    )
    whole_rows = sp_n * target_block
    kv_block = kv_block.reshape(source_block, 2, slot_heads, HEAD_DIM)
    keys, values = kv_block[:, 0], kv_block[:, 1]
    head_shape = (whole_rows, slot_heads, per_slot, HEAD_DIM)
    query_view = all_queries.reshape(head_shape)
    grad_view = all_grads.reshape(head_shape)

    scores = einsum("tgqd,sgd->gqts", query_view, keys) * score_scale
    part_max = jnp.max(scores, axis=-1)
    weights = jnp.exp(scores - part_max[..., None])
    part_total = jnp.sum(weights, axis=-1)
    d_probs = einsum("tgqd,sgd->gqts", grad_view, values)
    part_delta = jnp.sum(weights * d_probs, axis=-1)
    part_sum = einsum("gqts,sgd->tgqd", weights.astype(bf16), values)
    stats = jnp.stack([part_max, part_total, part_delta]).reshape(3 * local_heads, whole_rows)
    (all_stats,) = exchange(2, ("gather_sp", stats))
    all_stats = all_stats.reshape(sp_n, 3, slot_heads, per_slot, whole_rows)
    row_max = jnp.max(all_stats[:, 0], axis=0)
    rescale = jnp.exp(all_stats[:, 0] - row_max)
    total = jnp.sum(all_stats[:, 1] * rescale, axis=0)
    delta = jnp.sum(all_stats[:, 2] * rescale, axis=0) / total
    local_scale = jnp.exp(part_max - row_max) / total

    probs = weights * local_scale[..., None]
    d_scores = (probs * (d_probs - delta[..., None])).astype(bf16)
    value_sum = einsum("gqts,tgqd->sgd", probs.astype(bf16), grad_view)
    key_sum = einsum("gqts,tgqd->sgd", d_scores, query_view) * score_scale
    d_query = einsum("gqts,sgd->tgqd", d_scores, keys) * score_scale
    d_query = d_query.reshape(sp_n, target_block, local_width).astype(bf16)
    attended_part = part_sum * local_scale.transpose(2, 0, 1)[..., None]
    attended_part = attended_part.reshape(sp_n, target_block, local_width).astype(bf16)
    grads = jnp.concatenate(
        [key_sum.reshape(source_block, slot_width), value_sum.reshape(source_block, slot_width)],
        axis=1,
    )
    grads = grads.reshape(tp_n, source_local, 2 * slot_width).astype(bf16)
    query_terms, attended_terms, grads_back = exchange(
        3, ("swap_sp", d_query), ("swap_sp", attended_part), ("swap_tp", grads)
    )
    query_grad = jnp.sum(query_terms.astype(jnp.float32), axis=0).astype(bf16)
    attended = jnp.sum(attended_terms.astype(jnp.float32), axis=0).astype(bf16)

    target_terms = matmul(query_grad, query_weight.T).astype(bf16)
    target_back, attended_all = exchange(
        4,
        ("swap_tp", target_terms.reshape(tp_n, target_local, width)),
        ("gather_sp", attended),
    )

    def from_slots(matrix):
        folded = matrix.reshape(tp_n // copies, copies, source_local, slot_width)
        folded = jnp.sum(folded.astype(jnp.float32), axis=1)
        return folded.transpose(1, 0, 2).reshape(source_local, -1).astype(bf16)

    key_grad = from_slots(grads_back[:, :, :slot_width])
    value_grad = from_slots(grads_back[:, :, slot_width:])
    d_normed_s = matmul(key_grad, key_full.T) + matmul(value_grad, value_full.T)
    source_grad = norm_back(source_rows, source_gain, d_normed_s)
    d_normed_t = jnp.sum(target_back.astype(jnp.float32), axis=0)
    target_grad = out_cotangent.astype(jnp.float32) + norm_back(
        target_rows, target_gain, d_normed_t
    )
    attended_rows = attended_all.reshape(sp_n, tp_n, target_local, local_width)
    out_weight_grad = jnp.einsum(
        "stlw,tsld->wd", attended_rows, cot_all, preferred_element_type=jnp.float32
    )
    return (target_grad, source_grad, out_weight_grad)


def solution(mesh):
    return jax.shard_map(
        body,
        mesh=mesh,
        in_specs=(
            P(("sp", "tp"), None),
            P(("sp", "tp"), None),
            P(),
            P(),
            P(None, "tp"),
            P("tp", None),
            P("tp", None),
            P("tp", None),
            P(("sp", "tp"), None),
        ),
        out_specs=(P(("sp", "tp"), None), P(("sp", "tp"), None), P("tp", None)),
        check_vma=False,
    )
```

```python
import functools

import jax
import jax.numpy as jnp
from jax import lax
from jax.experimental import pallas as pl
from jax.experimental.pallas import tpu as pltpu
from jax.sharding import PartitionSpec as P

HEAD_DIM = 64
KV_HEADS = 8
EPSILON = 1e-06
MESH = pl.DeviceIdType.MESH


def normalize(matrix, gain_vector):
    widened = matrix.astype(jnp.float32)
    factor = lax.rsqrt(jnp.mean(widened * widened, axis=-1, keepdims=True) + EPSILON)
    return (widened * factor * gain_vector).astype(jnp.bfloat16)


def norm_back(matrix, gain_vector, upstream):
    widened = matrix.astype(jnp.float32)
    factor = lax.rsqrt(jnp.mean(widened * widened, axis=-1, keepdims=True) + EPSILON)
    weighted = upstream * gain_vector
    inner_sum = jnp.mean(weighted * widened, axis=-1, keepdims=True)
    return factor * weighted - widened * factor**3 * inner_sum


def exchange_kernel(kinds, sp_n, tp_n, *refs):
    count = len(kinds)
    ins, outs = refs[:count], refs[count : 2 * count]
    send_sems, recv_sems = refs[2 * count : 3 * count], refs[3 * count :]
    sp_me, tp_me = lax.axis_index("sp"), lax.axis_index("tp")
    sizes, places = {"sp": sp_n, "tp": tp_n}, {"sp": sp_me, "tp": tp_me}

    def address(axis, peer):
        return (peer, tp_me) if axis == "sp" else (sp_me, peer)

    axes = sorted({kind.split("_")[1] for kind in kinds})
    barrier = pltpu.get_barrier_semaphore()
    for axis in axes:
        for k in range(1, sizes[axis]):
            peer = lax.rem(places[axis] + k, sizes[axis])
            pl.semaphore_signal(barrier, inc=1, device_id=address(axis, peer), device_id_type=MESH)
    pl.semaphore_wait(barrier, sum(sizes[axis] - 1 for axis in axes))

    def copy(i, axis, source, slot, k, peer):
        return pltpu.make_async_remote_copy(
            src_ref=source,
            dst_ref=outs[i].at[slot],
            send_sem=send_sems[i].at[k],
            recv_sem=recv_sems[i].at[slot],
            device_id=address(axis, peer),
            device_id_type=MESH,
        )

    sent = []
    used = [0] * count

    def send(i, axis, source, target, recv, peer, keep=True):
        one = pltpu.make_async_remote_copy(
            src_ref=source,
            dst_ref=target,
            send_sem=send_sems[i].at[used[i]],
            recv_sem=recv_sems[i].at[recv],
            device_id=address(axis, peer),
            device_id_type=MESH,
        )
        used[i] += 1
        one.start()
        if keep:
            sent.append(one)
        return one

    def arrived(i, axis, target, recv):
        pltpu.make_async_remote_copy(
            src_ref=target,
            dst_ref=target,
            send_sem=send_sems[i].at[0],
            recv_sem=recv_sems[i].at[recv],
            device_id=address(axis, lax.rem(places[axis] + 1, sizes[axis])),
            device_id_type=MESH,
        ).wait_recv()

    square = tp_n == 8
    partner = tp_me + 1 - 2 * lax.rem(tp_me, 2)

    def across(index):
        return index + 2 - 4 * lax.rem(index // 2, 2)

    def along(index):
        return index + 4 - 8 * lax.rem(index // 4, 2)

    def relatives(index):
        if square:
            return [across(index), along(index)]
        return [lax.rem(index + 2 * k, tp_n) for k in range(1, tp_n // 2)]

    def forward(i, c, origin):
        chunks = ins[i].shape[0]
        piece, recv = outs[i].at[origin, c], origin * chunks + c
        arrived(i, "tp", piece, recv)
        send(i, "tp", piece, piece, recv, partner)
        return piece, recv

    line_sent = []
    depth = max([ins[i].shape[0] for i in range(count) if kinds[i] == "pair_tp"], default=0)
    for c in range(depth):
        for i, kind in enumerate(kinds):
            if kind == "pair_tp" and c < ins[i].shape[0]:
                chunks = ins[i].shape[0]
                for peer in relatives(tp_me) + [partner]:
                    piece = outs[i].at[tp_me, c]
                    send(i, "tp", ins[i].at[c], piece, tp_me * chunks + c, peer)
    for i, kind in enumerate(kinds):
        mode, axis = kind.split("_")
        n, me = sizes[axis], places[axis]
        if mode == "line":
            for step in (1, -1):
                inside = (me < n - 1) if step == 1 else (me > 0)
                line_sent.append((i, inside, used[i], me))

                @pl.when(inside)
                def _():
                    send(i, axis, ins[i], outs[i].at[me], me, me + step, keep=False)
        elif mode != "pair":
            for k in range(1, n):
                peer = lax.rem(me + k, n)
                source = ins[i] if mode == "gather" else ins[i].at[peer]
                send(i, axis, source, outs[i].at[me], me, peer)
    for i, kind in enumerate(kinds):
        mode, axis = kind.split("_")
        me = places[axis]
        outs[i][me] = ins[i][me] if mode == "swap" else ins[i][...]

    def line_step(i, far):
        n, me = sp_n, sp_me
        for step in (1, -1):
            origin = me - step * far
            valid = (origin >= 0) if step == 1 else (origin <= n - 1)
            onward = (valid & (me < n - 1)) if step == 1 else (valid & (me > 0))

            @pl.when(valid)
            def _():
                arrived(i, "sp", outs[i].at[origin], origin)

            if far < n - 1:
                line_sent.append((i, onward, used[i], origin))

                @pl.when(onward)
                def _():
                    piece = outs[i].at[origin]
                    send(i, "sp", piece, piece, origin, me + step, keep=False)

    def pair_step(i, c):
        me = tp_me
        chunks = ins[i].shape[0]
        for order, origin in enumerate(relatives(me)):
            piece, recv = forward(i, c, origin)
            if square and order == (i + c) % 2:
                send(i, "tp", piece, piece, recv, along(me) if order == 0 else across(me))

    lines = [i for i in range(count) if kinds[i] == "line_sp"]
    pairs = [i for i in range(count) if kinds[i] == "pair_tp"]
    for turn in range(max(depth, sp_n - 1 if lines else 0)):
        for i in pairs:
            if turn < ins[i].shape[0]:
                pair_step(i, turn)
        for i in lines:
            if turn + 1 < sp_n:
                line_step(i, turn + 1)
    if square:
        for c in range(depth):
            for i in pairs:
                if c < ins[i].shape[0]:
                    forward(i, c, across(along(tp_me)))
    for i, kind in enumerate(kinds):
        mode, axis = kind.split("_")
        n, me = sizes[axis], places[axis]
        if mode == "pair":
            chunks = ins[i].shape[0]
            others = relatives(partner) + ([across(along(partner))] if square else [])
            for origin in [partner] + others:
                for c in range(chunks):
                    arrived(i, axis, outs[i].at[origin, c], origin * chunks + c)
        elif mode != "line":
            for k in range(1, n):
                origin = lax.rem(me + n - k, n)
                arrived(i, axis, outs[i].at[origin], origin)
    for one in sent:
        one.wait_send()
    for i, happened, slot, origin in line_sent:

        @pl.when(happened)
        def _():
            pltpu.make_async_remote_copy(
                src_ref=outs[i].at[origin],
                dst_ref=outs[i].at[origin],
                send_sem=send_sems[i].at[slot],
                recv_sem=recv_sems[i].at[0],
                device_id=address("sp", lax.rem(sp_me + 1, sp_n)),
                device_id_type=MESH,
            ).wait_send()


def exchange(collective_id, *parts):
    sp_n, tp_n = lax.axis_size("sp"), lax.axis_size("tp")
    kinds = tuple(kind for kind, array in parts)
    arrays = [array for kind, array in parts]
    shapes, sends, recvs = [], [], []
    for kind, array in parts:
        mode, axis = kind.split("_")
        n = sp_n if axis == "sp" else tp_n
        shape = array.shape if mode == "swap" else (n,) + array.shape
        shapes.append(jax.ShapeDtypeStruct(shape, array.dtype))
        chunks = array.shape[0] if mode == "pair" else 1
        sends.append(pltpu.SemaphoreType.DMA(((2 * n + 8) * chunks,)))
        recvs.append(pltpu.SemaphoreType.DMA((n * chunks,)))
    return pl.pallas_call(
        functools.partial(exchange_kernel, kinds, sp_n, tp_n),
        out_shape=shapes,
        in_specs=[pl.BlockSpec(memory_space=pltpu.VMEM)] * len(parts),
        out_specs=[pl.BlockSpec(memory_space=pltpu.VMEM)] * len(parts),
        scratch_shapes=sends + recvs,
        compiler_params=pltpu.CompilerParams(
            collective_id=collective_id,
            has_side_effects=True,
            vmem_limit_bytes=56 * 1024 * 1024,
        ),
    )(*arrays)


def matmul(left, right):
    return jnp.dot(left, right, preferred_element_type=jnp.float32)


def einsum(text, left, right):
    return jnp.einsum(text, left, right, preferred_element_type=jnp.float32)


def body(
    target_rows,
    source_rows,
    target_gain,
    source_gain,
    query_weight,
    key_weight,
    value_weight,
    out_weight,
    out_cotangent,
):
    sp_n, tp_n = lax.axis_size("sp"), lax.axis_size("tp")
    width = target_rows.shape[1]
    local_width = query_weight.shape[1]
    local_heads = local_width // HEAD_DIM
    slot_heads = max(1, KV_HEADS // tp_n)
    copies = max(1, tp_n // KV_HEADS)
    per_slot = local_heads // slot_heads
    slot_width = slot_heads * HEAD_DIM
    score_scale = HEAD_DIM ** (-0.5)
    bf16 = jnp.bfloat16

    normed_t = normalize(target_rows, target_gain)
    normed_s = normalize(source_rows, source_gain)
    source_local = normed_s.shape[0]
    target_local = normed_t.shape[0]
    target_block = tp_n * target_local
    source_block = tp_n * source_local

    rows_in, cot_in, cot_column = exchange(
        0,
        ("pair_tp", normed_t[None]),
        ("pair_tp", out_cotangent[None]),
        ("line_sp", out_cotangent),
    )
    queries = matmul(rows_in.reshape(target_block, width), query_weight).astype(bf16)
    d_attended = matmul(cot_in.reshape(target_block, width), out_weight.T).astype(bf16)
    halves = (2, key_weight.shape[0] // 2, key_weight.shape[1])
    key_full, value_full, all_queries, all_grads = exchange(
        1,
        ("pair_tp", key_weight.reshape(halves)),
        ("pair_tp", value_weight.reshape(halves)),
        ("line_sp", queries),
        ("line_sp", d_attended),
    )
    key_full = key_full.reshape(width, -1)
    value_full = value_full.reshape(width, -1)
    key_own = matmul(normed_s, key_full).astype(bf16)
    value_own = matmul(normed_s, value_full).astype(bf16)

    def to_slots(matrix):
        split = matrix.reshape(source_local, tp_n // copies, 1, slot_width)
        spread = jnp.broadcast_to(split, (source_local, tp_n // copies, copies, slot_width))
        return spread.reshape(source_local, tp_n, slot_width).transpose(1, 0, 2)

    slots = jnp.concatenate([to_slots(key_own), to_slots(value_own)], axis=2)
    (kv_block,) = exchange(2, ("swap_tp", slots))
    whole_rows = sp_n * target_block
    kv_block = kv_block.reshape(source_block, 2, slot_heads, HEAD_DIM)
    keys, values = kv_block[:, 0], kv_block[:, 1]
    head_shape = (whole_rows, slot_heads, per_slot, HEAD_DIM)
    query_view = all_queries.reshape(head_shape)
    grad_view = all_grads.reshape(head_shape)

    scores = einsum("tgqd,sgd->gqts", query_view, keys) * score_scale
    part_max = jnp.max(scores, axis=-1)
    weights = jnp.exp(scores - part_max[..., None])
    part_total = jnp.sum(weights, axis=-1)
    d_probs = einsum("tgqd,sgd->gqts", grad_view, values)
    part_delta = jnp.sum(weights * d_probs, axis=-1)
    part_sum = einsum("gqts,sgd->tgqd", weights.astype(bf16), values)
    stats = jnp.stack([part_max, part_total, part_delta]).reshape(3 * local_heads, whole_rows)
    (all_stats,) = exchange(3, ("gather_sp", stats))
    all_stats = all_stats.reshape(sp_n, 3, slot_heads, per_slot, whole_rows)
    row_max = jnp.max(all_stats[:, 0], axis=0)
    rescale = jnp.exp(all_stats[:, 0] - row_max)
    total = jnp.sum(all_stats[:, 1] * rescale, axis=0)
    delta = jnp.sum(all_stats[:, 2] * rescale, axis=0) / total
    local_scale = jnp.exp(part_max - row_max) / total

    probs = weights * local_scale[..., None]
    d_scores = (probs * (d_probs - delta[..., None])).astype(bf16)
    value_sum = einsum("gqts,tgqd->sgd", probs.astype(bf16), grad_view)
    key_sum = einsum("gqts,tgqd->sgd", d_scores, query_view) * score_scale
    d_query = einsum("gqts,sgd->tgqd", d_scores, keys) * score_scale
    d_query = d_query.reshape(sp_n, target_block, local_width).astype(bf16)
    attended_part = part_sum * local_scale.transpose(2, 0, 1)[..., None]
    attended_part = attended_part.reshape(sp_n, target_block, local_width).astype(bf16)
    grads = jnp.concatenate(
        [key_sum.reshape(source_block, slot_width), value_sum.reshape(source_block, slot_width)],
        axis=1,
    )
    grads = grads.reshape(tp_n, source_local, 2 * slot_width).astype(bf16)
    query_terms, attended_terms, grads_back, cot_all = exchange(
        4,
        ("swap_sp", d_query),
        ("swap_sp", attended_part),
        ("swap_tp", grads),
        ("pair_tp", cot_column),
    )
    query_grad = jnp.sum(query_terms.astype(jnp.float32), axis=0).astype(bf16)
    attended = jnp.sum(attended_terms.astype(jnp.float32), axis=0).astype(bf16)

    target_terms = matmul(query_grad, query_weight.T).astype(bf16)
    target_back, attended_all = exchange(
        5,
        ("swap_tp", target_terms.reshape(tp_n, target_local, width)),
        ("line_sp", attended),
    )

    def from_slots(matrix):
        folded = matrix.reshape(tp_n // copies, copies, source_local, slot_width)
        folded = jnp.sum(folded.astype(jnp.float32), axis=1)
        return folded.transpose(1, 0, 2).reshape(source_local, -1).astype(bf16)

    key_grad = from_slots(grads_back[:, :, :slot_width])
    value_grad = from_slots(grads_back[:, :, slot_width:])
    d_normed_s = matmul(key_grad, key_full.T) + matmul(value_grad, value_full.T)
    source_grad = norm_back(source_rows, source_gain, d_normed_s)
    d_normed_t = jnp.sum(target_back.astype(jnp.float32), axis=0)
    target_grad = out_cotangent.astype(jnp.float32) + norm_back(
        target_rows, target_gain, d_normed_t
    )
    attended_rows = attended_all.reshape(sp_n, tp_n, target_local, local_width)
    out_weight_grad = jnp.einsum(
        "stlw,tsld->wd", attended_rows, cot_all, preferred_element_type=jnp.float32
    )
    return (target_grad, source_grad, out_weight_grad)


def solution(mesh):
    return jax.shard_map(
        body,
        mesh=mesh,
        in_specs=(
            P(("sp", "tp"), None),
            P(("sp", "tp"), None),
            P(),
            P(),
            P(None, "tp"),
            P("tp", None),
            P("tp", None),
            P("tp", None),
            P(("sp", "tp"), None),
        ),
        out_specs=(P(("sp", "tp"), None), P(("sp", "tp"), None), P("tp", None)),
        check_vma=False,
    )
```

```python
import functools

import jax
import jax.numpy as jnp
from jax import lax
from jax.experimental import pallas as pl
from jax.experimental.pallas import tpu as pltpu
from jax.sharding import PartitionSpec as P

HEAD_DIM = 64
KV_HEADS = 8
EPSILON = 1e-06
MESH = pl.DeviceIdType.MESH


def normalize(matrix, gain_vector):
    widened = matrix.astype(jnp.float32)
    factor = lax.rsqrt(jnp.mean(widened * widened, axis=-1, keepdims=True) + EPSILON)
    return (widened * factor * gain_vector).astype(jnp.bfloat16)


def norm_back(matrix, gain_vector, upstream):
    widened = matrix.astype(jnp.float32)
    factor = lax.rsqrt(jnp.mean(widened * widened, axis=-1, keepdims=True) + EPSILON)
    weighted = upstream * gain_vector
    inner_sum = jnp.mean(weighted * widened, axis=-1, keepdims=True)
    return factor * weighted - widened * factor**3 * inner_sum


def exchange_kernel(kinds, sp_n, tp_n, *refs):
    count = len(kinds)
    ins, outs = refs[:count], refs[count : 2 * count]
    send_sems, recv_sems = refs[2 * count : 3 * count], refs[3 * count :]
    sp_me, tp_me = lax.axis_index("sp"), lax.axis_index("tp")
    sizes, places = {"sp": sp_n, "tp": tp_n}, {"sp": sp_me, "tp": tp_me}

    def address(axis, peer):
        return (peer, tp_me) if axis == "sp" else (sp_me, peer)

    axes = sorted({kind.split("_")[1] for kind in kinds})
    barrier = pltpu.get_barrier_semaphore()
    for axis in axes:
        for k in range(1, sizes[axis]):
            peer = lax.rem(places[axis] + k, sizes[axis])
            pl.semaphore_signal(barrier, inc=1, device_id=address(axis, peer), device_id_type=MESH)
    pl.semaphore_wait(barrier, sum(sizes[axis] - 1 for axis in axes))

    def copy(i, axis, source, slot, k, peer):
        return pltpu.make_async_remote_copy(
            src_ref=source,
            dst_ref=outs[i].at[slot],
            send_sem=send_sems[i].at[k],
            recv_sem=recv_sems[i].at[slot],
            device_id=address(axis, peer),
            device_id_type=MESH,
        )

    sent = []
    used = [0] * count

    def send(i, axis, source, target, recv, peer, keep=True):
        one = pltpu.make_async_remote_copy(
            src_ref=source,
            dst_ref=target,
            send_sem=send_sems[i].at[used[i]],
            recv_sem=recv_sems[i].at[recv],
            device_id=address(axis, peer),
            device_id_type=MESH,
        )
        used[i] += 1
        one.start()
        if keep:
            sent.append(one)
        return one

    def arrived(i, axis, target, recv):
        pltpu.make_async_remote_copy(
            src_ref=target,
            dst_ref=target,
            send_sem=send_sems[i].at[0],
            recv_sem=recv_sems[i].at[recv],
            device_id=address(axis, lax.rem(places[axis] + 1, sizes[axis])),
            device_id_type=MESH,
        ).wait_recv()

    square = tp_n == 8
    partner = tp_me + 1 - 2 * lax.rem(tp_me, 2)

    def across(index):
        return index + 2 - 4 * lax.rem(index // 2, 2)

    def along(index):
        return index + 4 - 8 * lax.rem(index // 4, 2)

    def relatives(index):
        if square:
            return [across(index), along(index)]
        return [lax.rem(index + 2 * k, tp_n) for k in range(1, tp_n // 2)]

    def forward(i, c, origin):
        chunks = ins[i].shape[0]
        piece, recv = outs[i].at[origin, c], origin * chunks + c
        arrived(i, "tp", piece, recv)
        send(i, "tp", piece, piece, recv, partner)
        return piece, recv

    line_sent = []
    depth = max([ins[i].shape[0] for i in range(count) if kinds[i] == "pair_tp"], default=0)
    for c in range(depth):
        for i, kind in enumerate(kinds):
            if kind == "pair_tp" and c < ins[i].shape[0]:
                chunks = ins[i].shape[0]
                for peer in relatives(tp_me) + [partner]:
                    piece = outs[i].at[tp_me, c]
                    send(i, "tp", ins[i].at[c], piece, tp_me * chunks + c, peer)
    for i, kind in enumerate(kinds):
        mode, axis = kind.split("_")
        n, me = sizes[axis], places[axis]
        if mode == "line":
            for step in (1, -1):
                inside = (me < n - 1) if step == 1 else (me > 0)
                for c in range(ins[i].shape[0]):
                    line_sent.append((i, inside, used[i], me, c))
                    recv = me * ins[i].shape[0] + c

                    @pl.when(inside)
                    def _():
                        piece = outs[i].at[me, c]
                        send(i, axis, ins[i].at[c], piece, recv, me + step, keep=False)
        elif mode != "pair":
            for k in range(1, n):
                peer = lax.rem(me + k, n)
                source = ins[i] if mode == "gather" else ins[i].at[peer]
                send(i, axis, source, outs[i].at[me], me, peer)
    for i, kind in enumerate(kinds):
        mode, axis = kind.split("_")
        me = places[axis]
        outs[i][me] = ins[i][me] if mode == "swap" else ins[i][...]

    def line_step(i, far, c):
        n, me = sp_n, sp_me
        chunks = ins[i].shape[0]
        for step in (1, -1):
            origin = me - step * far
            valid = (origin >= 0) if step == 1 else (origin <= n - 1)
            onward = (valid & (me < n - 1)) if step == 1 else (valid & (me > 0))

            @pl.when(valid)
            def _():
                arrived(i, "sp", outs[i].at[origin, c], origin * chunks + c)

            if far < n - 1:
                line_sent.append((i, onward, used[i], origin, c))

                @pl.when(onward)
                def _():
                    piece = outs[i].at[origin, c]
                    recv = origin * chunks + c
                    send(i, "sp", piece, piece, recv, me + step, keep=False)

    def pair_step(i, c):
        me = tp_me
        chunks = ins[i].shape[0]
        for order, origin in enumerate(relatives(me)):
            piece, recv = forward(i, c, origin)
            if square and order == (i + c) % 2:
                send(i, "tp", piece, piece, recv, along(me) if order == 0 else across(me))

    lines = [i for i in range(count) if kinds[i] == "line_sp"]
    pairs = [i for i in range(count) if kinds[i] == "pair_tp"]
    for turn in range(max(depth, sp_n - 1 if lines else 0)):
        for i in pairs:
            if turn < ins[i].shape[0]:
                pair_step(i, turn)
        for i in lines:
            if turn + 1 < sp_n:
                for c in range(ins[i].shape[0]):
                    line_step(i, turn + 1, c)
    if square:
        for c in range(depth):
            for i in pairs:
                if c < ins[i].shape[0]:
                    forward(i, c, across(along(tp_me)))
    for i, kind in enumerate(kinds):
        mode, axis = kind.split("_")
        n, me = sizes[axis], places[axis]
        if mode == "pair":
            chunks = ins[i].shape[0]
            others = relatives(partner) + ([across(along(partner))] if square else [])
            for origin in [partner] + others:
                for c in range(chunks):
                    arrived(i, axis, outs[i].at[origin, c], origin * chunks + c)
        elif mode != "line":
            for k in range(1, n):
                origin = lax.rem(me + n - k, n)
                arrived(i, axis, outs[i].at[origin], origin)
    for one in sent:
        one.wait_send()
    for i, happened, slot, origin, c in line_sent:

        @pl.when(happened)
        def _():
            pltpu.make_async_remote_copy(
                src_ref=outs[i].at[origin, c],
                dst_ref=outs[i].at[origin, c],
                send_sem=send_sems[i].at[slot],
                recv_sem=recv_sems[i].at[0],
                device_id=address("sp", lax.rem(sp_me + 1, sp_n)),
                device_id_type=MESH,
            ).wait_send()


def exchange(collective_id, *parts):
    sp_n, tp_n = lax.axis_size("sp"), lax.axis_size("tp")
    kinds = tuple(kind for kind, array in parts)
    arrays = [array for kind, array in parts]
    shapes, sends, recvs = [], [], []
    for kind, array in parts:
        mode, axis = kind.split("_")
        n = sp_n if axis == "sp" else tp_n
        shape = array.shape if mode == "swap" else (n,) + array.shape
        shapes.append(jax.ShapeDtypeStruct(shape, array.dtype))
        chunks = array.shape[0] if mode in ("pair", "line") else 1
        sends.append(pltpu.SemaphoreType.DMA(((2 * n + 8) * chunks,)))
        recvs.append(pltpu.SemaphoreType.DMA((n * chunks,)))
    return pl.pallas_call(
        functools.partial(exchange_kernel, kinds, sp_n, tp_n),
        out_shape=shapes,
        in_specs=[pl.BlockSpec(memory_space=pltpu.VMEM)] * len(parts),
        out_specs=[pl.BlockSpec(memory_space=pltpu.VMEM)] * len(parts),
        scratch_shapes=sends + recvs,
        compiler_params=pltpu.CompilerParams(
            collective_id=collective_id,
            has_side_effects=True,
            vmem_limit_bytes=56 * 1024 * 1024,
        ),
    )(*arrays)


def matmul(left, right):
    return jnp.dot(left, right, preferred_element_type=jnp.float32)


def einsum(text, left, right):
    return jnp.einsum(text, left, right, preferred_element_type=jnp.float32)


def body(
    target_rows,
    source_rows,
    target_gain,
    source_gain,
    query_weight,
    key_weight,
    value_weight,
    out_weight,
    out_cotangent,
):
    sp_n, tp_n = lax.axis_size("sp"), lax.axis_size("tp")
    width = target_rows.shape[1]
    local_width = query_weight.shape[1]
    local_heads = local_width // HEAD_DIM
    slot_heads = max(1, KV_HEADS // tp_n)
    copies = max(1, tp_n // KV_HEADS)
    per_slot = local_heads // slot_heads
    slot_width = slot_heads * HEAD_DIM
    score_scale = HEAD_DIM ** (-0.5)
    bf16 = jnp.bfloat16

    normed_t = normalize(target_rows, target_gain)
    normed_s = normalize(source_rows, source_gain)
    source_local = normed_s.shape[0]
    target_local = normed_t.shape[0]
    target_block = tp_n * target_local
    source_block = tp_n * source_local

    rows_in, cot_in = exchange(
        0,
        ("pair_tp", normed_t[None]),
        ("pair_tp", out_cotangent[None]),
    )
    queries = matmul(rows_in.reshape(target_block, width), query_weight).astype(bf16)
    d_attended = matmul(cot_in.reshape(target_block, width), out_weight.T).astype(bf16)
    halves = (2, key_weight.shape[0] // 2, key_weight.shape[1])
    split = (2, target_block // 2, local_width)
    key_full, value_full, all_queries, all_grads, cot_column = exchange(
        1,
        ("pair_tp", key_weight.reshape(halves)),
        ("pair_tp", value_weight.reshape(halves)),
        ("line_sp", queries.reshape(split)),
        ("line_sp", d_attended.reshape(split)),
        ("line_sp", out_cotangent[None]),
    )
    key_full = key_full.reshape(width, -1)
    value_full = value_full.reshape(width, -1)
    key_own = matmul(normed_s, key_full).astype(bf16)
    value_own = matmul(normed_s, value_full).astype(bf16)

    def to_slots(matrix):
        split = matrix.reshape(source_local, tp_n // copies, 1, slot_width)
        spread = jnp.broadcast_to(split, (source_local, tp_n // copies, copies, slot_width))
        return spread.reshape(source_local, tp_n, slot_width).transpose(1, 0, 2)

    slots = jnp.concatenate([to_slots(key_own), to_slots(value_own)], axis=2)
    (kv_block,) = exchange(2, ("swap_tp", slots))
    whole_rows = sp_n * target_block
    kv_block = kv_block.reshape(source_block, 2, slot_heads, HEAD_DIM)
    keys, values = kv_block[:, 0], kv_block[:, 1]
    head_shape = (whole_rows, slot_heads, per_slot, HEAD_DIM)
    query_view = all_queries.reshape(head_shape)
    grad_view = all_grads.reshape(head_shape)

    scores = einsum("tgqd,sgd->gqts", query_view, keys) * score_scale
    part_max = jnp.max(scores, axis=-1)
    weights = jnp.exp(scores - part_max[..., None])
    part_total = jnp.sum(weights, axis=-1)
    d_probs = einsum("tgqd,sgd->gqts", grad_view, values)
    part_delta = jnp.sum(weights * d_probs, axis=-1)
    part_sum = einsum("gqts,sgd->tgqd", weights.astype(bf16), values)
    stats = jnp.stack([part_max, part_total, part_delta]).reshape(3 * local_heads, whole_rows)
    (all_stats,) = exchange(3, ("gather_sp", stats))
    all_stats = all_stats.reshape(sp_n, 3, slot_heads, per_slot, whole_rows)
    row_max = jnp.max(all_stats[:, 0], axis=0)
    rescale = jnp.exp(all_stats[:, 0] - row_max)
    total = jnp.sum(all_stats[:, 1] * rescale, axis=0)
    delta = jnp.sum(all_stats[:, 2] * rescale, axis=0) / total
    local_scale = jnp.exp(part_max - row_max) / total

    attended_part = part_sum * local_scale.transpose(2, 0, 1)[..., None]
    attended_part = attended_part.reshape(sp_n, target_block, local_width).astype(bf16)
    probs = weights * local_scale[..., None]
    d_scores = (probs * (d_probs - delta[..., None])).astype(bf16)
    value_sum = einsum("gqts,tgqd->sgd", probs.astype(bf16), grad_view)
    key_sum = einsum("gqts,tgqd->sgd", d_scores, query_view) * score_scale
    d_query = einsum("gqts,sgd->tgqd", d_scores, keys) * score_scale
    d_query = d_query.reshape(sp_n, target_block, local_width).astype(bf16)
    grads = jnp.concatenate(
        [key_sum.reshape(source_block, slot_width), value_sum.reshape(source_block, slot_width)],
        axis=1,
    )
    grads = grads.reshape(tp_n, source_local, 2 * slot_width).astype(bf16)
    query_terms, attended_terms, grads_back, cot_all = exchange(
        4,
        ("swap_sp", d_query),
        ("swap_sp", attended_part),
        ("swap_tp", grads),
        ("pair_tp", cot_column.reshape(sp_n, target_local, width)),
    )
    query_grad = jnp.sum(query_terms.astype(jnp.float32), axis=0).astype(bf16)
    attended = jnp.sum(attended_terms.astype(jnp.float32), axis=0).astype(bf16)

    target_terms = matmul(query_grad, query_weight.T).astype(bf16)
    target_back, attended_all = exchange(
        5,
        ("swap_tp", target_terms.reshape(tp_n, target_local, width)),
        ("line_sp", attended.reshape(split)),
    )

    def from_slots(matrix):
        folded = matrix.reshape(tp_n // copies, copies, source_local, slot_width)
        folded = jnp.sum(folded.astype(jnp.float32), axis=1)
        return folded.transpose(1, 0, 2).reshape(source_local, -1).astype(bf16)

    key_grad = from_slots(grads_back[:, :, :slot_width])
    value_grad = from_slots(grads_back[:, :, slot_width:])
    d_normed_s = matmul(key_grad, key_full.T) + matmul(value_grad, value_full.T)
    source_grad = norm_back(source_rows, source_gain, d_normed_s)
    d_normed_t = jnp.sum(target_back.astype(jnp.float32), axis=0)
    target_grad = out_cotangent.astype(jnp.float32) + norm_back(
        target_rows, target_gain, d_normed_t
    )
    attended_rows = attended_all.reshape(sp_n, tp_n, target_local, local_width)
    out_weight_grad = jnp.einsum(
        "stlw,tsld->wd", attended_rows, cot_all, preferred_element_type=jnp.float32
    )
    return (target_grad, source_grad, out_weight_grad)


def solution(mesh):
    return jax.shard_map(
        body,
        mesh=mesh,
        in_specs=(
            P(("sp", "tp"), None),
            P(("sp", "tp"), None),
            P(),
            P(),
            P(None, "tp"),
            P("tp", None),
            P("tp", None),
            P("tp", None),
            P(("sp", "tp"), None),
        ),
        out_specs=(P(("sp", "tp"), None), P(("sp", "tp"), None), P("tp", None)),
        check_vma=False,
    )
```
